32 devices in a mesh: fs: 8 (over z, y), tp: 4 (over x, core).
Axes of the slice: x: 2, y: 2, z: 4, core: 2. Of those that a mesh axis runs over, the one named last changes fastest.
Arguments:
- tokens: bfloat16 [6144, 2048], P('fs'), may hold values from -6 to 6
- norm_gain: float32 [2048], P('fs'), may hold values from 0.1 to 1.9
- gate_weight: float32 [2048, 5632], P('fs', 'tp'), may hold values from -0.125 to 0.125
- up_weight: float32 [2048, 5632], P('fs', 'tp'), may hold values from -0.125 to 0.125
- down_weight: float32 [5632, 2048], P('fs', 'tp'), may hold values from -0.078125 to 0.078125
Outputs:
- gate_out: bfloat16 [2048, 5632], P(None, 'tp')
- up_out: bfloat16 [2048, 5632], P(None, 'tp')
- down_out: bfloat16 [5632, 2048], P('tp')
- mixed: bfloat16 [6144, 2048], P('fs', 'tp')
The draws below stay inside these ranges and needn't reach their ends.
All inputs are finite; a program needn't handle non-finite values.
Results may differ from the reference program's by a relative error of at most 0.0095.
Values may be sent and summed in bfloat16 or wider, within the bound.
A program may use at most 128 MiB of HBM per device.

```python
import jax
import jax.numpy as jnp
from jax import lax

D = 2048
FF = 5632
TOKENS = 6144
N_TP = 4


def level_of(stream_key, dims, cuts, least, largest):
    gain, own = 1.0, jax.random.fold_in(stream_key, 6)
    for dim, blocks in cuts:
        heights = jnp.exp(jax.random.uniform(jax.random.fold_in(own, dim), (blocks,), jnp.float32, least / len(cuts), largest / len(cuts)))
        gain = gain * jnp.repeat(heights, dims[dim] // blocks).reshape([-1 if axis == dim else 1 for axis in range(len(dims))])
    return gain


def centred(rng, dims, width, reach, cuts=(), kind=jnp.bfloat16):
    result = width * jax.random.normal(rng, dims, jnp.float32)
    if cuts:
        result = result * level_of(rng, dims, cuts, -0.22, 0.18)
    return jnp.clip(result, -reach, reach).astype(kind)


def setup_inputs(seed: int = 0) -> dict:
    splits = jax.random.split(jax.random.key(seed), 6)
    return {
        "tokens": centred(splits[0], (TOKENS, D), 1.0, 6.0, ((0, 8),)),
        "norm_gain": jnp.clip(1.0 + 0.18 * jax.random.normal(splits[1], (D,), jnp.float32), 0.1, 1.9),
        "gate_weight": centred(splits[2], (D, FF), D ** -0.5, 0.125, ((0, 8), (1, 4)), jnp.float32),
        "up_weight": centred(splits[3], (D, FF), D ** -0.5, 0.125, ((0, 8), (1, 4)), jnp.float32),
        "down_weight": centred(splits[4], (FF, D), FF ** -0.5, 0.078125, ((0, 8), (1, 4)), jnp.float32),
    }


eps_norm = 1e-06

def reference(tokens, norm_gain, gate_weight, up_weight, down_weight):
    gain_column = norm_gain[:, None]
    gate_out = (gate_weight * gain_column).astype(jnp.bfloat16)
    up_out = (up_weight * gain_column).astype(jnp.bfloat16)
    down_out = down_weight.astype(jnp.bfloat16)
    rows_float = tokens.astype(jnp.float32)
    normed = (rows_float * lax.rsqrt(lax.optimization_barrier(jnp.mean(rows_float * rows_float, axis=-1, keepdims=True)) + eps_norm)).astype(jnp.bfloat16)
    gate_act = jnp.dot(normed, gate_out, preferred_element_type=jnp.float32)
    up_act = jnp.dot(normed, up_out, preferred_element_type=jnp.float32)
    hidden = (jax.nn.silu(gate_act) * up_act).astype(jnp.bfloat16)
    block_rows = FF // N_TP
    total = jnp.zeros((tokens.shape[0], D), jnp.float32)
    for index in range(N_TP):
        lower = index * block_rows
        share = jnp.dot(hidden[:, lower:lower + block_rows], down_out[lower:lower + block_rows, :], preferred_element_type=jnp.float32).astype(jnp.bfloat16)
        total = total + share.astype(jnp.float32)
    mixed = total.astype(jnp.bfloat16)
    return (gate_out, up_out, down_out, mixed)
```

```python
import functools

import jax
import jax.numpy as jnp
from jax import lax
from jax.experimental import pallas as pl
from jax.experimental.pallas import tpu as pltpu
from jax.sharding import PartitionSpec as P

eps_norm = 1e-06
MESH = pl.DeviceIdType.MESH

PIECES = (
    ("gate", 0, "a"),
    ("gate", 1, "a"),
    ("down", 1, "b"),
    ("up", 0, "a"),
    ("up", 1, "a"),
    ("down", 0, "a"),
)
PHASES = ((0, 1), (2,), (3, 4), (5,))


def plan(n_z):
    events = []
    seq = [(d, p) for phase in PHASES for d in range(1, n_z) for p in phase]
    own = {p: i + 1.0 for i, p in enumerate(range(len(PIECES)))}
    z_time, now = {}, 0.0
    for phase in PHASES:
        for d in range(1, n_z):
            for p in phase:
                if PIECES[p][2] == "a":
                    now += 1.0
                    z_time[d, p] = now
                    events.append((now, 0, "line", d, p))
                else:
                    now += 2.0
                    z_time[d, p] = now
                    events.append((now - 1.0, 0, "line", d, p))
                    events.append((now, 0, "line_other", d, p))
    y_time = {}
    for z in range(n_z):
        at = float(len(PIECES))
        for d, p in seq:
            if PIECES[p][2] == "a":
                for zz in (z - d, z + d):
                    if 0 <= zz < n_z:
                        at = max(at + 1.0, z_time[d, p] + 1.0)
                        y_time[d, p] = max(y_time.get((d, p), 0.0), at)
    for p, at in own.items():
        events.append((at, 1, "pair", 0, p))
    for (d, p), at in y_time.items():
        events.append((at, 1, "pair", d, p))
    here = dict(y_time)
    here.update({(0, p): at for p, at in own.items()})
    last = 0.0
    for name in ("gate", "up"):
        mine = [p for p in range(len(PIECES)) if PIECES[p][0] == name]
        for d in range(n_z):
            at = max(here[d, p] for p in mine) + 0.01
            events.append((at, 2, "mul_" + name, d, 0))
            last = max(last, at)
    events.append((last + 0.01, 3, "act", 0, 0))
    return sorted(events)


def kernel(
    n_fs, n_tp, tok, gain, gw, uw, dw, gate_o, up_o, down_o, mix_o,
    dcol, normed, acc_g, acc_u, hidden, share, half_in, out_send, out_in,
    ag_send, ag_recv, aa_send, aa_recv, rs_send, rs_recv,
):
    f, t = lax.axis_index("fs"), lax.axis_index("tp")
    n_z = n_fs // 2
    z, y = f // 2, f % 2
    per = n_fs // n_tp
    rows = gw.shape[0]
    d_rows, d_cols = dw.shape
    half = d_cols // 2
    n_tok = tok.shape[0]
    k_z = normed.shape[2]
    m_tile = min(256, n_tok)
    width = gw.shape[1]
    col_tiles = [(c, min(512, width - c)) for c in range(0, width, 512)]

    def flip(bit):
        return t + bit - 2 * bit * ((t // bit) % 2)

    near, far = flip(1), flip(2)
    far_near = far + 1 - 2 * (far % 2)

    def view(o, p):
        name, h, _ = PIECES[p]
        if name == "down":
            return dcol.at[o, :, pl.ds(h * half, half)]
        ref = gate_o if name == "gate" else up_o
        return ref.at[pl.ds(pl.multiple_of(o * rows + h * (rows // 2), rows // 2), rows // 2), :]

    def ag(o, p, way, dest):
        v = view(o, p)
        return pltpu.make_async_remote_copy(
            v, v, ag_send.at[o, p, way], ag_recv.at[o, p],
            device_id=(dest, t), device_id_type=MESH,
        )

    started = []

    def start(cond, make):
        if cond is None:
            make().start()
        else:
            pl.when(cond)(lambda: make().start())
        started.append((cond, make))

    def land(o, p):
        ag(o, p, 0, f).wait_recv()

    def exchange(cond, o, p):
        name, h, _ = PIECES[p]
        if name != "down":
            return
        owner = o // per
        k = o % per
        row = pl.multiple_of(k * d_rows, d_rows)
        col = pl.multiple_of(t * d_cols + h * half, half)

        def make():
            return pltpu.make_async_remote_copy(
                view(o, p), down_o.at[pl.ds(row, d_rows), pl.ds(col, half)],
                aa_send.at[o, h], aa_recv.at[t, k, h],
                device_id=(f, owner), device_id_type=MESH,
            )

        away = owner != t
        start(away if cond is None else jnp.logical_and(cond, away), make)
        mine = owner == t

        @pl.when(mine if cond is None else jnp.logical_and(cond, mine))
        def _():
            down_o[pl.ds(row, d_rows), pl.ds(col, half)] = dcol[o, :, h * half : (h + 1) * half]

    barrier = pltpu.get_barrier_semaphore()
    other_y = f + 1 - 2 * y
    peers = [
        (z > 0, (f - 2, t)), (z < n_z - 1, (f + 2, t)), (None, (other_y, t)),
        (None, (f, near)), (None, (f, far)), (None, (f, far_near)),
    ]
    for cond, dev in peers:
        def hello(dev=dev):
            pl.semaphore_signal(barrier, inc=1, device_id=dev, device_id_type=MESH)
        hello() if cond is None else pl.when(cond)(hello)

    g = gain[...]
    base = pl.multiple_of(f * rows, rows)
    gate_o[pl.ds(base, rows), :] = (gw[...] * g).astype(jnp.bfloat16)
    dcol[f] = dw[...].astype(jnp.bfloat16)
    up_o[pl.ds(base, rows), :] = (uw[...] * g).astype(jnp.bfloat16)
    inner = jnp.logical_and(z > 0, z < n_z - 1)
    pl.when(inner)(lambda: pl.semaphore_wait(barrier, len(peers)))
    pl.when(jnp.logical_not(inner))(lambda: pl.semaphore_wait(barrier, len(peers) - 1))

    for p in range(len(PIECES)):
        start(z > 0, functools.partial(ag, f, p, 0, f - 2))
        start(z < n_z - 1, functools.partial(ag, f, p, 1, f + 2))
        start(None, functools.partial(ag, f, p, 2, other_y))
    for p in range(len(PIECES)):
        exchange(None, f, p)

    n_norm = n_tok // 64

    @pl.loop(0, n_norm)
    def _(i):
        r = pl.multiple_of(i * 64, 64)
        x = tok[pl.ds(r, 64), :].astype(jnp.float32)
        x = x * lax.rsqrt(jnp.mean(x * x, axis=-1, keepdims=True) + eps_norm)
        x = x.astype(jnp.bfloat16)
        for j in range(n_z):
            normed[j, pl.ds(r, 64), :] = x[:, j * k_z : (j + 1) * k_z]

    def multiply(w, acc, zz, first):
        k0 = pl.multiple_of(zz * k_z, k_z)

        @pl.loop(0, n_tok // m_tile)
        def _(i):
            r = pl.multiple_of(i * m_tile, m_tile)
            a = normed[zz, pl.ds(r, m_tile), :]
            for c, n in col_tiles:
                v = jnp.dot(a, w[pl.ds(k0, k_z), c : c + n], preferred_element_type=jnp.float32)
                if first:
                    acc[pl.ds(r, m_tile), c : c + n] = v
                else:
                    acc[pl.ds(r, m_tile), c : c + n] += v

    def sides(d):
        return [(z >= d, z - d, -1), (z + d < n_z, z + d, 1)]

    def forward(cond, zz, sign, o, p):
        if sign < 0:
            start(jnp.logical_and(cond, z < n_z - 1), functools.partial(ag, o, p, 1, f + 2))
        else:
            start(jnp.logical_and(cond, z > 0), functools.partial(ag, o, p, 0, f - 2))

    def halves(h):
        k_tile = 256

        def aa_wait(c):
            for k in range(per):
                pltpu.make_async_remote_copy(
                    down_o.at[pl.ds(k * d_rows, d_rows), pl.ds(0, half)],
                    down_o.at[pl.ds(k * d_rows, d_rows), pl.ds(pl.multiple_of(c * d_cols + h * half, half), half)],
                    aa_send.at[0, h], aa_recv.at[c, k, h], device_id=(f, near), device_id_type=MESH,
                ).wait_recv()

        def product(c, slot):
            @pl.loop(0, n_tok // m_tile)
            def _(i):
                r = pl.multiple_of(i * m_tile, m_tile)
                col = pl.multiple_of(c * d_cols + h * half, half)
                v = jnp.dot(hidden[pl.ds(r, m_tile), :], down_o[:, pl.ds(col, half)], preferred_element_type=jnp.float32)
                share[h, slot, pl.ds(r, m_tile), :] = v.astype(jnp.bfloat16)

        def pair(slot):
            return pltpu.make_async_remote_copy(
                share.at[h, slot], half_in.at[h, slot], rs_send.at[h, slot], rs_recv.at[h, slot],
                device_id=(f, near), device_id_type=MESH,
            )

        def across():
            return pltpu.make_async_remote_copy(
                out_send.at[h], out_in.at[h], rs_send.at[h, 2], rs_recv.at[h, 2],
                device_id=(f, far), device_id_type=MESH,
            )

        aa_wait(far_near)
        product(far_near, 0)
        start(None, functools.partial(pair, 0))
        aa_wait(far)
        product(far, 2)
        pair(0).wait_recv()
        out_send[h] = (share[h, 2].astype(jnp.float32) + half_in[h, 0].astype(jnp.float32)).astype(jnp.bfloat16)
        start(None, across)
        aa_wait(near)
        product(near, 1)
        start(None, functools.partial(pair, 1))
        product(t, 3)

        def finish():
            pair(1).wait_recv()
            across().wait_recv()
            mix_o[:, h * half : (h + 1) * half] = (
                share[h, 3].astype(jnp.float32) + half_in[h, 1].astype(jnp.float32) + out_in[h].astype(jnp.float32)
            ).astype(jnp.bfloat16)

        return finish

    for _, _, what, d, p in plan(n_z):
        if what == "line":
            for cond, zz, sign in sides(d):
                o = zz * 2 + y
                pl.when(cond)(functools.partial(land, o, p))
                forward(cond, zz, sign, o, p)
                if PIECES[p][2] == "a":
                    start(cond, functools.partial(ag, o, p, 2, other_y))
                exchange(cond, o, p)
        elif what == "line_other":
            for cond, zz, sign in sides(d):
                o = zz * 2 + 1 - y
                pl.when(cond)(functools.partial(land, o, p))
                forward(cond, zz, sign, o, p)
                exchange(cond, o, p)
        elif what == "pair":
            if d == 0:
                land(other_y, p)
                if PIECES[p][2] == "b":
                    start(z > 0, functools.partial(ag, other_y, p, 0, f - 2))
                    start(z < n_z - 1, functools.partial(ag, other_y, p, 1, f + 2))
                exchange(None, other_y, p)
            else:
                for cond, zz, sign in sides(d):
                    o = zz * 2 + 1 - y
                    pl.when(cond)(functools.partial(land, o, p))
                    exchange(cond, o, p)
        elif what == "mul_gate" or what == "mul_up":
            w, acc = (gate_o, acc_g) if what == "mul_gate" else (up_o, acc_u)
            if d == 0:
                multiply(w, acc, z, True)
            else:
                for cond, zz, sign in sides(d):
                    pl.when(cond)(functools.partial(multiply, w, acc, zz, False))
        elif what == "act":
            @pl.loop(0, n_tok // 32)
            def _(i):
                r = pl.multiple_of(i * 32, 32)
                v = acc_g[pl.ds(r, 32), :]
                hidden[pl.ds(r, 32), :] = (v / (1.0 + jnp.exp(-v)) * acc_u[pl.ds(r, 32), :]).astype(jnp.bfloat16)

    first = halves(1)
    second = halves(0)
    first()
    second()
    for cond, make in started:
        if cond is None:
            make().wait_send()
        else:
            pl.when(cond)(lambda make=make: make().wait_send())


def on_device(n_fs, n_tp, tokens, norm_gain, gate_weight, up_weight, down_weight):
    n_tok, d_model = tokens.shape
    rows, width = gate_weight.shape
    d_rows, d_cols = down_weight.shape
    half = d_cols // 2
    n_z = n_fs // 2
    n_p = len(PIECES)
    bf = jnp.bfloat16
    vmem = pl.BlockSpec(memory_space=pltpu.VMEM)
    dma = pltpu.SemaphoreType.DMA
    return pl.pallas_call(
        functools.partial(kernel, n_fs, n_tp),
        out_shape=(
            jax.ShapeDtypeStruct((d_model, width), bf),
            jax.ShapeDtypeStruct((d_model, width), bf),
            jax.ShapeDtypeStruct((d_rows * n_fs // n_tp, d_model), bf),
            jax.ShapeDtypeStruct((n_tok, d_cols), bf),
        ),
        in_specs=[vmem] * 5,
        out_specs=(vmem,) * 4,
        scratch_shapes=[
            pltpu.VMEM((n_fs, d_rows, d_cols), bf),
            pltpu.VMEM((n_z, n_tok, d_model // n_z), bf),
            pltpu.VMEM((n_tok, width), jnp.float32),
            pltpu.VMEM((n_tok, width), jnp.float32),
            pltpu.VMEM((n_tok, width), bf),
            pltpu.VMEM((2, 4, n_tok, half), bf),
            pltpu.VMEM((2, 2, n_tok, half), bf),
            pltpu.VMEM((2, n_tok, half), bf),
            pltpu.VMEM((2, n_tok, half), bf),
            dma((n_fs, n_p, 3)),
            dma((n_fs, n_p)),
            dma((n_fs, 2)),
            dma((n_tp, n_fs // n_tp, 2)),
            dma((2, 3)),
            dma((2, 3)),
        ],
        compiler_params=pltpu.CompilerParams(
            collective_id=0, has_side_effects=True, vmem_limit_bytes=67043328
        ),
    )(tokens, norm_gain[:, None], gate_weight, up_weight, down_weight)


def solution(mesh):
    n_fs, n_tp = mesh.shape["fs"], mesh.shape["tp"]
    in_specs = (P("fs", None), P("fs"), P("fs", "tp"), P("fs", "tp"), P("fs", "tp"))
    out_specs = (P(None, "tp"), P(None, "tp"), P("tp", None), P("fs", "tp"))
    return jax.shard_map(
        functools.partial(on_device, n_fs, n_tp), mesh=mesh, in_specs=in_specs, out_specs=out_specs, check_vma=False
    )
```

```python
import functools

import jax
import jax.numpy as jnp
from jax import lax
from jax.experimental import pallas as pl
from jax.experimental.pallas import tpu as pltpu
from jax.sharding import PartitionSpec as P

eps_norm = 1e-06
MESH = pl.DeviceIdType.MESH

PIECES = (
    ("gate", 0, 1, "a"),
    ("gate", 1, 1, "a"),
    ("down", 2, 2, "b"),
    ("up", 0, 1, "a"),
    ("up", 1, 1, "a"),
    ("down", 0, 1, "a"),
    ("down", 1, 1, "a"),
)
PHASES = ((0, 1, 6), (2,), (3, 4), (5,))
GROUPS = ((1, 3, (2, 6)), (0, 1, (5,)))


def cost(p):
    return 0.5 if PIECES[p][0] == "down" and kind(p) == 1 else 1.0


def kind(p):
    return PIECES[p][3]


def plan(n_z):
    events = []
    seq = [(d, p) for phase in PHASES for d in range(1, n_z) for p in phase]
    order = sorted(range(len(PIECES)), key=lambda p: kind(p) == "a")
    own, total = {}, 0.0
    for p in order:
        total += cost(p)
        own[p] = total
    z_time, now = {}, 0.0
    for i, phase in enumerate(PHASES):
        for d in range(1, n_z):
            if d == n_z - 1 and i + 1 < len(PHASES):
                events.append((now + 0.02, 1, "launch", i + 1, 0))
            for p in phase:
                if kind(p) == "a":
                    now += cost(p)
                    z_time[d, p] = now
                    events.append((now, 0, "line", d, p))
                else:
                    now += 2.0 * cost(p)
                    z_time[d, p] = now
                    events.append((now - cost(p), 0, "line", d, p))
                    events.append((now, 0, "line_other", d, p))
    y_time = {}
    for z in range(n_z):
        at = total
        for d, p in seq:
            if kind(p) == "a":
                for zz in (z - d, z + d):
                    if 0 <= zz < n_z:
                        at = max(at, z_time[d, p]) + cost(p)
                        y_time[d, p] = max(y_time.get((d, p), 0.0), at)
    for p, at in own.items():
        events.append((at, 1, "pair", 0, p))
    for (d, p), at in y_time.items():
        events.append((at, 1, "pair", d, p))
    here = dict(y_time)
    here.update({(0, p): at for p, at in own.items()})
    last = 0.0
    for name in ("gate", "up"):
        mine = [p for p in range(len(PIECES)) if PIECES[p][0] == name]
        for d in range(n_z):
            at = max(here[d, p] for p in mine) + 0.01
            events.append((at, 2, "mul_" + name, d, 0))
            last = max(last, at)
    events.append((last + 0.01, 3, "act", 0, 0))
    end = max(e[0] for e in events) + 0.1
    for step in range(4):
        events.append((end + 0.01 + 0.01 * step, 4, "share", 0, step))
    for step in range(5):
        events.append((end + 0.1 + 0.1 * step, 4, "share", 1, step))
    events.append((end + 0.35, 4, "share", 0, 4))
    return sorted(events)


def kernel(
    n_fs, n_tp, tok_hbm, gain, gw, uw, dw, gate_o, up_o, down_o, mix_o,
    tok, dcol, normed, acc_g, acc_u, hidden, share0, share1, pair0, pair1, send0, send1, in0, in1,
    tok_sem, ag_send, ag_recv, aa_send, aa_recv, rs_send, rs_recv,
):
    tok_copy = pltpu.make_async_copy(tok_hbm, tok, tok_sem)
    tok_copy.start()
    shares, pairs, sends, ins = (share0, share1), (pair0, pair1), (send0, send1), (in0, in1)
    f, t = lax.axis_index("fs"), lax.axis_index("tp")
    n_z = n_fs // 2
    z, y = f // 2, f % 2
    per = n_fs // n_tp
    rows = gw.shape[0]
    d_rows, d_cols = dw.shape
    part = d_cols // 4
    n_tok = tok.shape[0]
    k_z = normed.shape[2]
    m_tile = min(256, n_tok)
    width = gw.shape[1]
    col_tiles = [(c, min(512, width - c)) for c in range(0, width, 512)]

    def flip(bit):
        return t + bit - 2 * bit * ((t // bit) % 2)

    near, far = flip(1), flip(2)
    far_near = far + 1 - 2 * (far % 2)

    def view(o, p):
        name, h, n, _ = PIECES[p]
        if name == "down":
            return dcol.at[o, :, pl.ds(h * part, n * part)]
        ref = gate_o if name == "gate" else up_o
        return ref.at[pl.ds(pl.multiple_of(o * rows + h * (rows // 2), rows // 2), rows // 2), :]

    def ag(o, p, way, dest):
        v = view(o, p)
        return pltpu.make_async_remote_copy(
            v, v, ag_send.at[o, p, way], ag_recv.at[o, p],
            device_id=(dest, t), device_id_type=MESH,
        )

    started = []

    def start(cond, make):
        if cond is None:
            make().start()
        else:
            pl.when(cond)(lambda: make().start())
        started.append((cond, make))

    def land(o, p):
        ag(o, p, 0, f).wait_recv()

    def exchange(cond, o, p):
        name, h, n, _ = PIECES[p]
        if name != "down":
            return
        owner = o // per
        k = o % per
        row = pl.multiple_of(k * d_rows, d_rows)
        col = pl.multiple_of(t * d_cols + h * part, part)

        def make():
            return pltpu.make_async_remote_copy(
                view(o, p), down_o.at[pl.ds(row, d_rows), pl.ds(col, n * part)],
                aa_send.at[o, p], aa_recv.at[t, k, p],
                device_id=(f, owner), device_id_type=MESH,
            )

        away = owner != t
        start(away if cond is None else jnp.logical_and(cond, away), make)
        mine = owner == t

        @pl.when(mine if cond is None else jnp.logical_and(cond, mine))
        def _():
            down_o[pl.ds(row, d_rows), pl.ds(col, n * part)] = dcol[o, :, h * part : (h + n) * part]

    barrier = pltpu.get_barrier_semaphore()
    other_y = f + 1 - 2 * y
    peers = [
        (z > 0, (f - 2, t)), (z < n_z - 1, (f + 2, t)), (None, (other_y, t)),
        (None, (f, near)), (None, (f, far)), (None, (f, far_near)),
    ]
    for cond, dev in peers:
        def hello(dev=dev):
            pl.semaphore_signal(barrier, inc=1, device_id=dev, device_id_type=MESH)
        hello() if cond is None else pl.when(cond)(hello)

    g = jnp.broadcast_to(gain[...], (8, rows)).T[:, :1]
    base = pl.multiple_of(f * rows, rows)
    gate_o[pl.ds(base, rows), :] = (gw[...] * g).astype(jnp.bfloat16)
    dcol[f] = dw[...].astype(jnp.bfloat16)
    up_o[pl.ds(base, rows), :] = (uw[...] * g).astype(jnp.bfloat16)
    inner = jnp.logical_and(z > 0, z < n_z - 1)
    pl.when(inner)(lambda: pl.semaphore_wait(barrier, len(peers)))
    pl.when(jnp.logical_not(inner))(lambda: pl.semaphore_wait(barrier, len(peers) - 1))

    def launch(phase):
        for p in PHASES[phase]:
            start(z > 0, functools.partial(ag, f, p, 0, f - 2))
            start(z < n_z - 1, functools.partial(ag, f, p, 1, f + 2))
            if kind(p) == "b":
                other_b(p)

    def other_b(p):
        start(z > 0, functools.partial(ag, other_y, p, 0, f - 2))
        start(z < n_z - 1, functools.partial(ag, other_y, p, 1, f + 2))

    for p in sorted(range(len(PIECES)), key=lambda p: kind(p) == "a"):
        start(None, functools.partial(ag, f, p, 2, other_y))
    for p in PHASES[0]:
        start(z > 0, functools.partial(ag, f, p, 0, f - 2))
        start(z < n_z - 1, functools.partial(ag, f, p, 1, f + 2))
    for p in range(len(PIECES)):
        exchange(None, f, p)

    n_norm = n_tok // 64
    tok_copy.wait()

    @pl.loop(0, n_norm)
    def _(i):
        r = pl.multiple_of(i * 64, 64)
        x = tok[pl.ds(r, 64), :].astype(jnp.float32)
        x = x * lax.rsqrt(jnp.mean(x * x, axis=-1, keepdims=True) + eps_norm)
        x = x.astype(jnp.bfloat16)
        for j in range(n_z):
            normed[j, pl.ds(r, 64), :] = x[:, j * k_z : (j + 1) * k_z]

    def multiply(w, acc, zz, first):
        k0 = pl.multiple_of(zz * k_z, k_z)

        @pl.loop(0, n_tok // m_tile)
        def _(i):
            r = pl.multiple_of(i * m_tile, m_tile)
            a = normed[zz, pl.ds(r, m_tile), :]
            for c, n in col_tiles:
                v = jnp.dot(a, w[pl.ds(k0, k_z), c : c + n], preferred_element_type=jnp.float32)
                if first:
                    acc[pl.ds(r, m_tile), c : c + n] = v
                else:
                    acc[pl.ds(r, m_tile), c : c + n] += v

    def sides(d):
        return [(z >= d, z - d, -1), (z + d < n_z, z + d, 1)]

    def forward(cond, zz, sign, o, p):
        if sign < 0:
            start(jnp.logical_and(cond, z < n_z - 1), functools.partial(ag, o, p, 1, f + 2))
        else:
            start(jnp.logical_and(cond, z > 0), functools.partial(ag, o, p, 0, f - 2))

    def share_step(group, step):
        q, n, parts = GROUPS[group]
        share, half_in, out_send, out_in = shares[group], pairs[group], sends[group], ins[group]
        wide = n * part

        def aa_wait(c):
            for k in range(per):
                for p in parts:
                    _, h, m, _ = PIECES[p]
                    ref = down_o.at[
                        pl.ds(k * d_rows, d_rows), pl.ds(pl.multiple_of(c * d_cols + h * part, part), m * part)
                    ]
                    pltpu.make_async_remote_copy(
                        ref, ref, aa_send.at[0, p], aa_recv.at[c, k, p], device_id=(f, near), device_id_type=MESH,
                    ).wait_recv()

        def product(c, slot):
            @pl.loop(0, n_tok // m_tile)
            def _(i):
                r = pl.multiple_of(i * m_tile, m_tile)
                col = pl.multiple_of(c * d_cols + q * part, part)
                v = jnp.dot(hidden[pl.ds(r, m_tile), :], down_o[:, pl.ds(col, wide)], preferred_element_type=jnp.float32)
                share[slot, pl.ds(r, m_tile), :] = v.astype(jnp.bfloat16)

        def pair(slot):
            return pltpu.make_async_remote_copy(
                share.at[slot], half_in.at[slot], rs_send.at[group, slot], rs_recv.at[group, slot],
                device_id=(f, near), device_id_type=MESH,
            )

        def across():
            return pltpu.make_async_remote_copy(
                out_send, out_in, rs_send.at[group, 2], rs_recv.at[group, 2],
                device_id=(f, far), device_id_type=MESH,
            )

        if step == 0:
            aa_wait(far_near)
            product(far_near, 0)
            start(None, functools.partial(pair, 0))
        elif step == 1:
            aa_wait(far)
            product(far, 2)
            pair(0).wait_recv()
            out_send[...] = (share[2].astype(jnp.float32) + half_in[0].astype(jnp.float32)).astype(jnp.bfloat16)
            start(None, across)
        elif step == 2:
            aa_wait(near)
            product(near, 1)
            start(None, functools.partial(pair, 1))
        elif step == 3:
            product(t, 3)
        elif step == 4:
            pair(1).wait_recv()
            across().wait_recv()
            mix_o[:, q * part : (q + n) * part] = (
                share[3].astype(jnp.float32) + half_in[1].astype(jnp.float32) + out_in[...].astype(jnp.float32)
            ).astype(jnp.bfloat16)

    for _, _, what, d, p in plan(n_z):
        if what == "launch":
            launch(d)
        elif what == "share":
            share_step(d, p)
        elif what == "line":
            for cond, zz, sign in sides(d):
                o = zz * 2 + y
                pl.when(cond)(functools.partial(land, o, p))
                forward(cond, zz, sign, o, p)
                if kind(p) == "a":
                    start(cond, functools.partial(ag, o, p, 2, other_y))
                exchange(cond, o, p)
        elif what == "line_other":
            for cond, zz, sign in sides(d):
                o = zz * 2 + 1 - y
                pl.when(cond)(functools.partial(land, o, p))
                forward(cond, zz, sign, o, p)
                exchange(cond, o, p)
        elif what == "pair":
            if d == 0:
                land(other_y, p)
                exchange(None, other_y, p)
            else:
                for cond, zz, sign in sides(d):
                    o = zz * 2 + 1 - y
                    pl.when(cond)(functools.partial(land, o, p))
                    exchange(cond, o, p)
        elif what == "mul_gate" or what == "mul_up":
            w, acc = (gate_o, acc_g) if what == "mul_gate" else (up_o, acc_u)
            if d == 0:
                multiply(w, acc, z, True)
            else:
                for cond, zz, sign in sides(d):
                    pl.when(cond)(functools.partial(multiply, w, acc, zz, False))
        elif what == "act":
            @pl.loop(0, n_tok // 32)
            def _(i):
                r = pl.multiple_of(i * 32, 32)
                v = acc_g[pl.ds(r, 32), :]
                hidden[pl.ds(r, 32), :] = (v / (1.0 + jnp.exp(-v)) * acc_u[pl.ds(r, 32), :]).astype(jnp.bfloat16)

    for cond, make in started:
        if cond is None:
            make().wait_send()
        else:
            pl.when(cond)(lambda make=make: make().wait_send())


def on_device(n_fs, n_tp, tokens, norm_gain, gate_weight, up_weight, down_weight):
    n_tok, d_model = tokens.shape
    rows, width = gate_weight.shape
    d_rows, d_cols = down_weight.shape
    part = d_cols // 4
    n_z = n_fs // 2
    n_p = len(PIECES)
    bf = jnp.bfloat16
    vmem = pl.BlockSpec(memory_space=pltpu.VMEM)
    dma = pltpu.SemaphoreType.DMA
    return pl.pallas_call(
        functools.partial(kernel, n_fs, n_tp),
        out_shape=(
            pltpu.VMEM((d_model, width), bf),
            pltpu.VMEM((d_model, width), bf),
            pltpu.VMEM((d_rows * n_fs // n_tp, d_model), bf),
            pltpu.VMEM((n_tok, d_cols), bf),
        ),
        in_specs=[pl.BlockSpec(memory_space=pl.ANY)] + [vmem] * 4,
        out_specs=(vmem,) * 4,
        scratch_shapes=[
            pltpu.VMEM((n_tok, d_model), bf),
            pltpu.VMEM((n_fs, d_rows, d_cols), bf),
            pltpu.VMEM((n_z, n_tok, d_model // n_z), bf),
            pltpu.VMEM((n_tok, width), jnp.float32),
            pltpu.VMEM((n_tok, width), jnp.float32),
            pltpu.VMEM((n_tok, width), bf),
            *[pltpu.VMEM((4, n_tok, g[1] * part), bf) for g in GROUPS],
            *[pltpu.VMEM((2, n_tok, g[1] * part), bf) for g in GROUPS],
            *[pltpu.VMEM((n_tok, g[1] * part), bf) for g in GROUPS],
            *[pltpu.VMEM((n_tok, g[1] * part), bf) for g in GROUPS],
            dma,
            dma((n_fs, n_p, 3)),
            dma((n_fs, n_p)),
            dma((n_fs, n_p)),
            dma((n_tp, n_fs // n_tp, n_p)),
            dma((2, 3)),
            dma((2, 3)),
        ],
        compiler_params=pltpu.CompilerParams(
            collective_id=0, has_side_effects=True, vmem_limit_bytes=46 * 2**20
        ),
    )(tokens, norm_gain[None, :], gate_weight, up_weight, down_weight)


def solution(mesh):
    n_fs, n_tp = mesh.shape["fs"], mesh.shape["tp"]
    in_specs = (P("fs", None), P("fs"), P("fs", "tp"), P("fs", "tp"), P("fs", "tp"))
    out_specs = (P(None, "tp"), P(None, "tp"), P("tp", None), P("fs", "tp"))
    return jax.shard_map(
        functools.partial(on_device, n_fs, n_tp), mesh=mesh, in_specs=in_specs, out_specs=out_specs, check_vma=False
    )
```
